32 devices in a mesh: sp: 8 (over z, x), tp: 4 (over y, core).
Axes of the slice: x: 2, y: 2, z: 4, core: 2. Of those that a mesh axis runs over, the one named last changes fastest.
Arguments:
- stream_in: bfloat16 [2048, 2048], P(('sp', 'tp')), may hold values from -6 to 6
- queries: bfloat16 [2048, 4096], P('sp', 'tp'), may hold values from -6 to 6
- key_rows: bfloat16 [2048, 4096], P('sp', 'tp'), may hold values from -6 to 6
- values: bfloat16 [2048, 8192], P('sp', 'tp'), may hold values from -6 to 6
- decay_low: bfloat16 [2048, 16], P('sp'), may hold values from -4 to 4
- decay_matrix: bfloat16 [16, 4096], P(None, 'tp'), may hold values from -1.5 to 1.5
- decay_bias: float32 [4096], P('tp')
- decay_shift: float32 [2048, 16], P('sp', 'tp'), may hold values from -1 to 0
- head_gain: float32 [512], replicated, may hold values from 0.1 to 1.9
- output_matrix: bfloat16 [8192, 2048], P('tp'), may hold values from -0.0625 to 0.0625
- feed_gain: float32 [2048], replicated, may hold values from 0.1 to 1.9
- routes: int32 [2048, 2], P('sp'), may hold values from 0 to 7, all different within a row; in each aligned block of 256 rows (0 to 255, 256 to 511, ...) at most 64 rows name the same one
- route_weights: float32 [2048, 2], P('sp'), may hold values from 0.2 to 1
- expert_gate: bfloat16 [8, 2048, 2816], P('sp', None, 'tp'), may hold values from -0.125 to 0.125
- specialist_widen: bfloat16 [8, 2048, 2816], P('sp', None, 'tp'), may hold values from -0.125 to 0.125
- expert_down: bfloat16 [8, 2816, 2048], P('sp', 'tp'), may hold values from -0.109375 to 0.109375
Outputs:
- layer_out: bfloat16 [2048, 2048], P(('sp', 'tp'))
The draws below stay inside these ranges and needn't reach their ends.
Inputs may be any that keep to these rules, and one draw needn't show every extreme that they name: `routes`: each row names 2 different experts; within each aligned block of 256 rows no expert is named by more than 64 rows, and in every draw some expert is named by exactly 64 rows of some block.
All inputs are finite; a program needn't handle non-finite values.
Results may differ from the reference program's by a relative error of at most 0.02.
Values may be sent and summed in bfloat16 or wider, within the bound.
A program may use at most 128 MiB of HBM per device.

```python
import math
import jax
import jax.numpy as jnp
import numpy as np
from jax import lax

D = 2048
HEADS = 16
HK = 256
HV = 512
RANK = 16
FF = 2816
TOP = 2
BLK = 128
TOK_DEV = 256
SEQUENCE_LENGTH = 2048
EXPERTS = 8
CAPG = 64
N_SP = 8
N_TP = 4


def draw_decay_bias(key, part):
    key_pick = jax.random.fold_in(key, 11)
    key_slow = jax.random.fold_in(key, 12)
    key_fast = jax.random.fold_in(key, 13)
    fast_heads = jax.random.uniform(key_pick, (HEADS,), jnp.float32) < 0.5
    slow_values = jnp.log(jnp.float32(SEQUENCE_LENGTH)) + 1.0 + jax.random.uniform(key_slow, (HEADS, HK), jnp.float32, 0.0, 1.5)
    fast_values = jax.random.uniform(key_fast, (HEADS, HK), jnp.float32, -0.5, 1.0)
    return jnp.where(fast_heads[:, None], fast_values, slow_values).reshape(HEADS * HK).astype(jnp.float32)


def draw_decay_shift(key, part):
    key_rate = jax.random.fold_in(key, 21)
    key_where = jax.random.fold_in(key, 22)
    key_loss = jax.random.fold_in(key, 23)
    blocks = SEQUENCE_LENGTH // TOK_DEV
    rates = jnp.exp(jax.random.uniform(key_rate, (blocks, HEADS), jnp.float32, jnp.log(0.25), 0.0)) * (-1.5 / SEQUENCE_LENGTH)
    averaging_coefficient = jnp.repeat(rates, TOK_DEV, axis=0)
    places = jax.random.randint(key_where, (2, HEADS), 0, SEQUENCE_LENGTH)
    objective_readings = jnp.log(jax.random.uniform(key_loss, (2, HEADS), jnp.float32, 0.5, 0.8))
    positions = jnp.arange(SEQUENCE_LENGTH, dtype=jnp.int32)
    overflow_entries = (positions[:, None, None] == places[None, :, :]).astype(jnp.float32)
    cluster_batches = jnp.sum(overflow_entries * objective_readings[None, :, :], axis=1)
    return (averaging_coefficient + cluster_batches).astype(jnp.float32)


def steps_of(stream_key, shape, cuts, smallest, high):
    level = 1.0
    for dim, blocks in cuts:
        steps = jax.random.uniform(jax.random.fold_in(jax.random.fold_in(stream_key, 6), dim), (blocks,), jnp.float32, smallest / len(cuts), high / len(cuts))
        level = level * jnp.repeat(jnp.exp(steps), shape[dim] // blocks).reshape((-1,) + (1,) * (len(shape) - 1 - dim))
    return level


def assign_block(own_key, own, number, rows, amount, top, bound, skew):
    ranking = jax.random.permutation(own_key, amount)
    crowded, usual = portions_of(amount, rows * top, bound, skew, True), portions_of(amount, rows * top, bound, skew, False)
    places = jnp.arange(amount)

    def named(tallies, offset_by):
        used = int((tallies > 0).sum())
        fixed = max(1, used // 4)
        moved = fixed + (places - fixed + offset_by * (used - fixed)) % max(1, amount - fixed)
        return jnp.zeros((amount,), jnp.int32).at[ranking[jnp.where(places < fixed, places, moved)]].set(jnp.asarray(tallies, jnp.int32))

    tallies = jnp.where(number % 4 == 0, named(crowded, number // 4), named(usual, number - number // 4 - 1))
    mixed = jax.random.permutation(jax.random.fold_in(own, 3), amount)
    source_of, receiver = mixed[0:amount // 2 * 2:2], mixed[1:amount // 2 * 2:2]
    slack = jnp.minimum(tallies[source_of] - 1, bound - tallies[receiver]) // 2
    slack = jnp.where((source_of == ranking[0]) | (receiver == ranking[0]) | (tallies[receiver] == 0), 0, jnp.maximum(slack, 0))
    moved = jax.random.randint(jax.random.fold_in(own, 4), (amount // 2,), 0, 1 << 20) % (slack + 1)
    tallies = tallies.at[source_of].add(-moved).at[receiver].add(moved)
    members = jnp.searchsorted(jnp.cumsum(tallies), jnp.arange(rows * top), side="right").astype(jnp.int32)
    grid = members.reshape(top, rows).T
    grid = grid[jax.random.permutation(jax.random.fold_in(own, 1), rows)]
    offset_by = jax.random.randint(jax.random.fold_in(own, 2), (rows, 1), 0, top)
    return jnp.take_along_axis(grid, (jnp.arange(top)[None, :] + offset_by) % top, axis=1)


def portions_of(number_of, total, reach, skew, full):
    weights = [(1 << 20) // math.isqrt(rank ** skew) + 1 for rank in range(1, number_of + 1)]
    largest = reach if full else min(reach, max(-(-total // number_of), total * weights[0] // sum(weights)))
    least = 1 if total - largest >= number_of - 1 else 0
    given, surplus = [largest] + [least] * (number_of - 1), total - largest - least * (number_of - 1)
    while surplus > 0:
        free = [i for i in range(1, number_of) if given[i] < largest] or [i for i in range(1, number_of) if given[i] < reach]
        whole, remaining = sum([weights[i] for i in free]), surplus
        for i in free:
            more = min(reach - given[i], max(1, remaining * weights[i] // whole), surplus)
            given[i] = given[i] + more
            surplus = surplus - more
    return np.array(given)


def normal_values(own_key, shape, spread, most, shards=(), held_as=jnp.bfloat16):
    drawn = jax.random.normal(own_key, shape, jnp.float32) * spread
    if len(shards) > 0:
        drawn = steps_of(own_key, shape, shards, -0.22, 0.18) * drawn
    return jnp.clip(drawn, min=-most, max=most).astype(held_as)


def setup_inputs(seed: int = 0) -> dict:
    splits = jax.random.split(jax.random.key(seed), 17)
    stream_in = normal_values(splits[0], (SEQUENCE_LENGTH, D), 1.0, 6.0, ((0, 32),))
    queries = normal_values(splits[1], (SEQUENCE_LENGTH, HEADS * HK), 1.0, 6.0, ((0, 8), (1, 4)))
    key_rows = normal_values(splits[2], (SEQUENCE_LENGTH, HEADS * HK), 1.0, 6.0, ((0, 8), (1, 4)))
    values = normal_values(splits[3], (SEQUENCE_LENGTH, HEADS * HV), 1.0, 6.0, ((0, 8), (1, 4)))
    decay_low = normal_values(splits[4], (SEQUENCE_LENGTH, RANK), 1.0, 4.0, ((0, 8),))
    decay_matrix = normal_values(splits[5], (RANK, HEADS * HK), RANK ** -0.5, 1.5, ((1, 4),))
    decay_bias = draw_decay_bias(jax.random.fold_in(splits[16], 71), 0)
    decay_shift = draw_decay_shift(jax.random.fold_in(splits[16], 71), 0)
    head_gain = jnp.clip(1.0 + 0.18 * jax.random.normal(splits[8], (HV,), jnp.float32), 0.1, 1.9)
    output_matrix = normal_values(splits[9], (HEADS * HV, D), (HEADS * HV) ** -0.5, 0.0625, ((0, 4),))
    feed_gain = jnp.clip(1.0 + 0.18 * jax.random.normal(splits[10], (D,), jnp.float32), 0.1, 1.9)
    routes_keys = jax.random.split(jax.random.fold_in(splits[11], 1), SEQUENCE_LENGTH // TOK_DEV)
    routes_turns = jax.random.permutation(jax.random.fold_in(splits[11], 3), SEQUENCE_LENGTH // TOK_DEV)
    routes = jax.vmap(lambda own, number: assign_block(jax.random.fold_in(splits[11], 2), own, number, TOK_DEV, EXPERTS, TOP, CAPG, 0))(routes_keys, routes_turns).reshape((SEQUENCE_LENGTH, TOP))
    route_weights = jnp.clip(0.2 + 0.8 * jax.random.uniform(splits[12], (SEQUENCE_LENGTH, TOP), jnp.float32) ** steps_of(splits[12], (SEQUENCE_LENGTH, TOP), ((0, 8),), -0.2, 0.2), 0.2, 1.0)
    expert_gate = normal_values(splits[13], (EXPERTS, D, FF), D ** -0.5, 0.125, ((0, 8), (2, 4)))
    specialist_widen = normal_values(splits[14], (EXPERTS, D, FF), D ** -0.5, 0.125, ((0, 8), (2, 4)))
    expert_down = normal_values(splits[15], (EXPERTS, FF, D), FF ** -0.5, 0.109375, ((0, 8), (1, 4)))
    return {"stream_in": stream_in, "queries": queries, "key_rows": key_rows, "values": values, "decay_low": decay_low, "decay_matrix": decay_matrix, "decay_bias": decay_bias, "decay_shift": decay_shift, "head_gain": head_gain, "output_matrix": output_matrix, "feed_gain": feed_gain, "routes": routes, "route_weights": route_weights, "expert_gate": expert_gate, "specialist_widen": specialist_widen, "expert_down": expert_down}


TEMPER = 16.0
EPSILON = 1e-06
HIGHEST = lax.Precision.HIGHEST

def decay_logs(decay_low, decay_matrix, decay_bias, decay_shift, heads):
    before_gate = jnp.dot(decay_low, decay_matrix, preferred_element_type=jnp.float32) + decay_bias
    logged = jax.nn.log_sigmoid(before_gate) / TEMPER
    return logged.reshape(before_gate.shape[0], heads, HK) + decay_shift[:, :, None]

def into_blocks(array):
    length, heads, width = array.shape
    return array.reshape(length // BLK, BLK, heads, width).transpose(2, 0, 1, 3)

def segment_summands(queries, key_rows, values, log_decay):
    inside = jnp.cumsum(log_decay, axis=2)
    final_position = inside[:, :, -1:, :]
    scaled_query = queries * jnp.exp(inside) * HK ** (-0.5)
    scaled_key = key_rows * jnp.exp(-inside)
    end_keys = key_rows * jnp.exp(final_position - inside)
    scores = jnp.einsum('hnid,hnjd->hnij', scaled_query, scaled_key, precision=HIGHEST)
    causal = jnp.tril(jnp.ones((BLK, BLK), jnp.bool_))
    scores = jnp.where(causal, scores, 0.0)
    local_out = jnp.einsum('hnij,hnjv->hniv', scores, values, precision=HIGHEST)
    partial_update = jnp.einsum('hnjd,hnjv->hndv', end_keys, values, precision=HIGHEST)
    return (scaled_query, local_out, partial_update, jnp.exp(final_position[:, :, 0, :]))

def run_blocks(scaled_query, partial_update, block_decay, start):

    def advance(state, pieces):
        query_block, added, decay = pieces
        output = jnp.einsum('hid,hdv->hiv', query_block, state, precision=HIGHEST)
        return (state * decay[:, :, None] + added, output)
    final, outputs = lax.scan(advance, start, (jnp.moveaxis(scaled_query, 1, 0), jnp.moveaxis(partial_update, 1, 0), jnp.moveaxis(block_decay, 1, 0)))
    return (final, jnp.moveaxis(outputs, 0, 1))

def head_norm(heads_out, head_gain):
    heads = heads_out.shape[0]
    flat = heads_out.transpose(1, 2, 0, 3).reshape(-1, heads, HV)
    normed = flat * lax.rsqrt(lax.optimization_barrier(jnp.mean(flat * flat, axis=-1, keepdims=True)) + EPSILON) * head_gain
    return normed.reshape(-1, heads * HV).astype(jnp.bfloat16)

def root_scale(midstream, gain):
    return (midstream * lax.rsqrt(lax.optimization_barrier(jnp.mean(midstream * midstream, axis=-1, keepdims=True)) + EPSILON) * gain).astype(jnp.bfloat16)

def reference(stream_in, queries, key_rows, values, decay_low, decay_matrix, decay_bias, decay_shift, head_gain, output_matrix, feed_gain, routes, route_weights, expert_gate, specialist_widen, expert_down):
    log_decay = decay_logs(decay_low, decay_matrix, decay_bias, decay_shift, HEADS)

    def shaped(array, width):
        return into_blocks(array.astype(jnp.float32).reshape(SEQUENCE_LENGTH, HEADS, width))
    scaled_query, local_out, partial_update, block_decay = segment_summands(shaped(queries, HK), shaped(key_rows, HK), shaped(values, HV), into_blocks(log_decay))
    start = jnp.zeros((HEADS, HK, HV), jnp.float32)
    _, carried_out = run_blocks(scaled_query, partial_update, block_decay, start)
    mixed = head_norm(local_out + carried_out, head_gain)
    group_width = HEADS * HV // N_TP
    mixed_groups = mixed.reshape(SEQUENCE_LENGTH, N_TP, group_width).transpose(1, 0, 2)
    matrix_groups = output_matrix.reshape(N_TP, group_width, D)

    def group_step(total, inputs):
        rows_group, matrix_group = inputs
        product = jnp.dot(rows_group, matrix_group, preferred_element_type=jnp.float32)
        rounded = lax.optimization_barrier(product.astype(jnp.bfloat16))
        return (total + rounded.astype(jnp.float32), None)
    attended, _ = lax.scan(group_step, jnp.zeros((SEQUENCE_LENGTH, D), jnp.float32), (mixed_groups, matrix_groups))
    midstream = stream_in.astype(jnp.float32) + attended
    normed = root_scale(midstream, feed_gain)
    slots = N_SP * CAPG
    flat_routes = routes.reshape(-1)
    flat_weights = route_weights.reshape(-1)
    piece = FF // N_TP

    def expert_step(total, inputs):
        expert, gate_matrix, up_matrix, down_projection_weight = inputs
        matches = flat_routes == expert
        chosen = jnp.nonzero(matches, size=slots, fill_value=0)[0].astype(jnp.int32)
        live = (jnp.arange(slots, dtype=jnp.int32) < jnp.sum(matches.astype(jnp.int32))).astype(jnp.float32)
        token_index = chosen // TOP
        picked = normed[token_index]
        gated = jnp.dot(picked, gate_matrix, preferred_element_type=jnp.float32)
        lifted = jnp.dot(picked, up_matrix, preferred_element_type=jnp.float32)
        hidden = (jax.nn.silu(gated) * lifted).astype(jnp.bfloat16)
        pieces = jnp.einsum('rpf,pfd->prd', hidden.reshape(slots, N_TP, piece).astype(jnp.float32), down_projection_weight.reshape(N_TP, piece, D).astype(jnp.float32))
        rounded = lax.optimization_barrier(pieces.astype(jnp.bfloat16))
        expert_token_rows = lax.optimization_barrier(jnp.sum(rounded.astype(jnp.float32), axis=0)).astype(jnp.bfloat16)
        term = expert_token_rows.astype(jnp.float32) * (flat_weights[chosen] * live)[:, None]
        return (total.at[token_index].add(term), None)
    routed, _ = lax.scan(expert_step, jnp.zeros((SEQUENCE_LENGTH, D), jnp.float32), (jnp.arange(EXPERTS, dtype=jnp.int32), expert_gate, specialist_widen, expert_down))
    return (midstream + routed).astype(jnp.bfloat16)
```

```python
import functools

import jax
import jax.numpy as jnp
from jax import lax
from jax.experimental import pallas as pl
from jax.experimental.pallas import tpu as pltpu
from jax.sharding import PartitionSpec as P

HK = 256
HV = 512
TOP = 2
BLK = 128
TEMPER = 16.0
EPSILON = 1e-06
HIGHEST = lax.Precision.HIGHEST
MESH = pl.DeviceIdType.MESH
F32 = jnp.float32
BF16 = jnp.bfloat16


def mm(a, b, ca, cb, precision=None):
    return lax.dot_general(
        a, b, (((ca,), (cb,)), ((), ())), preferred_element_type=F32, precision=precision
    )


def remote(src, dst, send, recv, target):
    return pltpu.make_async_remote_copy(
        src_ref=src, dst_ref=dst, send_sem=send, recv_sem=recv, device_id=target, device_id_type=MESH
    )


def scatter_sum(src, r1, half, r2, s1, q1, s2, q2, y, c, ny, sent):
    partner = {"tp": 2 * y + 1 - c}
    for i in range(1, ny + 1):
        to = lax.rem(y + i, ny)
        copy = remote(src.at[to, 1 - c], r1.at[to], s1.at[to], q1.at[to], partner)
        copy.start()
        sent.append(copy)
    for i in range(1, ny):
        to = lax.rem(y + i, ny)
        remote(src.at[to, c], r1.at[to], s1.at[to], q1.at[to], partner).wait_recv()
        half[to] = (src[to, c].astype(F32) + r1[to].astype(F32)).astype(BF16)
        copy = remote(half.at[to], r2.at[y], s2.at[to], q2.at[y], {"tp": 2 * to + c})
        copy.start()
        sent.append(copy)
    remote(src.at[y, c], r1.at[y], s1.at[y], q1.at[y], partner).wait_recv()
    total = src[y, c].astype(F32) + r1[y].astype(F32)
    for i in range(1, ny):
        to = lax.rem(y + i, ny)
        remote(half.at[to], r2.at[to], s2.at[to], q2.at[to], {"tp": 2 * to + c}).wait_recv()
        total = total + r2[to].astype(F32)
    return total


def layer_kernel(
    n, nt, hs,
    stream, q, k, v, low, mat, bias, shift, gain, wout, fgain, routes, rweights, wgate, wup, wdown,
    out,
    ins, prior, sbuf, rbuf, cbuf, carry, dec, decall, acc, qs,
    wo, wg, wu, wd, mixed,
    prod, p1, ph, p2, mid, group, selt, wcomb, fb, rows, pb, r4, hb, r5, part, t1, th, t2,
    wsem, sa, ra, sd, rd, sb, rb, sp1, rp1, sp2, rp2, sg, rg, sgc, rgc, sx, rx, sxc, rxc,
    s4, q4, s5, q5, st1, rt1, st2, rt2,
):
    me = lax.axis_index("sp")
    t = lax.axis_index("tp")
    y = t // 2
    c = lax.rem(t, 2)
    ny = nt // 2
    partner = {"tp": 2 * y + 1 - c}
    length = q.shape[0]
    heads = q.shape[1] // HK
    blocks = length // BLK
    width = stream.shape[1]
    rows_here = stream.shape[0]
    sent = []

    barrier = pltpu.get_barrier_semaphore()
    for i in range(1, n):
        pl.semaphore_signal(barrier, inc=1, device_id={"sp": lax.rem(me + i, n)}, device_id_type=MESH)
    for i in range(1, ny):
        pl.semaphore_signal(
            barrier, inc=1, device_id={"tp": 2 * lax.rem(y + i, ny) + c}, device_id_type=MESH
        )
    pl.semaphore_signal(barrier, inc=1, device_id=partner, device_id_type=MESH)

    loads = [
        pltpu.make_async_copy(wout, wo, wsem.at[0]),
        pltpu.make_async_copy(wgate.at[0], wg, wsem.at[1]),
        pltpu.make_async_copy(wup.at[0], wu, wsem.at[2]),
        pltpu.make_async_copy(wdown.at[0], wd, wsem.at[3]),
    ]
    for load in loads:
        load.start()

    row_id = lax.broadcasted_iota(jnp.int32, (BLK, BLK), 0)
    col_id = lax.broadcasted_iota(jnp.int32, (BLK, BLK), 1)
    causal = row_id >= col_id
    tril = causal.astype(F32)

    for h in range(heads):
        ks, vs = slice(h * HK, (h + 1) * HK), slice(h * HV, (h + 1) * HV)
        pre = mm(low[...], mat[:, ks], 1, 0) + bias[:, ks]
        logged = (jnp.minimum(pre, 0.0) - jnp.log1p(jnp.exp(-jnp.abs(pre)))) / TEMPER + shift[:, h : h + 1]
        state = None
        whole = None
        for b in range(blocks):
            at = slice(b * BLK, (b + 1) * BLK)
            inside = mm(tril, logged[at], 1, 0, HIGHEST)
            ins[at, ks] = inside
            last = inside[BLK - 1 : BLK, :]
            end = (k[at, ks].astype(F32) * jnp.exp(last - inside)).astype(BF16)
            added = mm(v[at, vs], end, 0, 0)
            state = added if state is None else state * jnp.exp(last) + added
            whole = last if whole is None else whole + last
            if b < blocks - 1:
                prior[b, :, ks] = state.astype(BF16)
        sbuf[:, :, ks] = state.astype(BF16).reshape(n, HV // n, HK)
        dec[:, ks] = jnp.exp(whole)

    pl.semaphore_wait(barrier, n - 1 + ny - 1 + 1)
    for i in range(1, n):
        to = lax.rem(me + i, n)
        copy = remote(dec, decall.at[me], sd.at[to], rd.at[me], {"sp": to})
        copy.start()
        sent.append(copy)
        copy = remote(sbuf.at[to], rbuf.at[me], sa.at[to], ra.at[me], {"sp": to})
        copy.start()
        sent.append(copy)
    rbuf[me] = sbuf[me]
    decall[me] = dec[...]

    for h in range(heads):
        ks, vs = slice(h * HK, (h + 1) * HK), slice(h * HV, (h + 1) * HV)
        passed = None
        for b in range(blocks):
            at = slice(b * BLK, (b + 1) * BLK)
            inside = ins[at, ks]
            last = inside[BLK - 1 : BLK, :]
            centre = last * 0.5
            qf = q[at, ks].astype(F32) * HK ** (-0.5)
            sq = (qf * jnp.exp(inside - centre)).astype(BF16)
            sk = (k[at, ks].astype(F32) * jnp.exp(centre - inside)).astype(BF16)
            scores = jnp.where(causal, mm(sq, sk, 1, 1), 0.0).astype(BF16)
            local = mm(scores, v[at, vs], 1, 0)
            full = inside if passed is None else inside + passed
            qs[at, ks] = (qf * jnp.exp(full)).astype(BF16)
            if b > 0:
                local = local + mm((qf * jnp.exp(inside)).astype(BF16), prior[b - 1, :, ks], 1, 1)
            passed = last if passed is None else passed + last
            acc[at, vs] = local

    total = jnp.zeros((HV // n, heads * HK), F32)
    for j in range(n):
        cbuf[j] = total.astype(BF16)

        @pl.when(j != me)
        def _():
            remote(cbuf.at[j], carry.at[me], sb.at[j], rb.at[me], {"sp": j}).start()
            remote(dec, decall.at[j], sd.at[j], rd.at[j], {"sp": j}).wait_recv()
            remote(sbuf.at[j], rbuf.at[j], sa.at[j], ra.at[j], {"sp": j}).wait_recv()

        total = total * decall[j] + rbuf[j].astype(F32)
    carry[me] = cbuf[me]

    lane = lax.broadcasted_iota(jnp.int32, (length, n), 1)
    first = (routes[:, 0:1] == lane).astype(F32)
    second = (routes[:, 1:2] == lane).astype(F32)
    earlier = (
        lax.broadcasted_iota(jnp.int32, (length, length), 0)
        > lax.broadcasted_iota(jnp.int32, (length, length), 1)
    ).astype(BF16)
    counts = mm(earlier, (first + second).astype(BF16), 1, 0)
    slot_lane = lax.broadcasted_iota(jnp.int32, (length, n * hs), 1).astype(F32)
    base = (c * hs).astype(F32)
    chosen = jnp.zeros((length, n * hs), F32)
    weighted = jnp.zeros((length, n * hs), F32)
    for j, mask in enumerate((first, second)):
        rank = jnp.sum(counts * mask, axis=1, keepdims=True) - base
        place = jnp.where(
            (rank >= 0) & (rank < hs), routes[:, j : j + 1].astype(F32) * hs + rank, -1.0
        )
        hit = place == slot_lane
        chosen = chosen + jnp.where(hit, 1.0, 0.0)
        weighted = weighted + jnp.where(hit, rweights[:, j : j + 1], 0.0)
    selt[...] = chosen.astype(BF16)
    wcomb[...] = weighted.astype(BF16)

    for i in range(1, n):
        j = lax.rem(me + i, n)
        remote(cbuf.at[j], carry.at[j], sb.at[j], rb.at[j], {"sp": j}).wait()
    for h in range(heads):
        ks, vs = slice(h * HK, (h + 1) * HK), slice(h * HV, (h + 1) * HV)
        x = acc[:, vs] + mm(qs[:, ks], carry[:, :, ks].reshape(HV, HK), 1, 1)
        scale = lax.rsqrt(jnp.mean(x * x, axis=-1, keepdims=True) + EPSILON)
        mixed[:, vs] = (x * scale * gain[...]).astype(BF16)

    loads[0].wait()
    tile = 256

    @pl.loop(0, width // tile)
    def _(i):
        at = pl.ds(pl.multiple_of(i * tile, tile), tile)
        piece = mm(mixed[...], wo[:, at], 1, 0).astype(BF16)
        prod[:, :, :, at] = piece.reshape(ny, 2, rows_here, tile)

    attended = scatter_sum(prod, p1, ph, p2, sp1, rp1, sp2, rp2, y, c, ny, sent)
    midstream = stream[...].astype(F32) + attended
    mid[...] = midstream
    scale = lax.rsqrt(jnp.mean(midstream * midstream, axis=-1, keepdims=True) + EPSILON)
    group[y, c] = (midstream * scale * fgain[...]).astype(BF16)

    for i in range(1, ny):
        to = lax.rem(y + i, ny)
        copy = remote(group.at[y, c], group.at[y, c], sg.at[to], rg.at[y], {"tp": 2 * to + c})
        copy.start()
        sent.append(copy)
    copy = remote(group.at[y, c], group.at[y, c], sgc.at[y], rgc.at[y], partner)
    copy.start()
    sent.append(copy)
    for i in range(1, ny):
        to = lax.rem(y + i, ny)
        remote(group.at[to, c], group.at[to, c], sg.at[to], rg.at[to], {"tp": 2 * to + c}).wait_recv()
        copy = remote(group.at[to, c], group.at[to, c], sgc.at[to], rgc.at[to], partner)
        copy.start()
        sent.append(copy)
    for i in range(ny):
        to = lax.rem(y + i, ny)
        remote(group.at[to, 1 - c], group.at[to, 1 - c], sgc.at[to], rgc.at[to], partner).wait_recv()

    @pl.loop(0, width // tile)
    def _(i):
        at = pl.ds(pl.multiple_of(i * tile, tile), tile)
        picked = mm(selt[...], group[:, :, :, at].reshape(length, tile), 0, 0)
        fb[:, :, at] = picked.astype(BF16).reshape(n, hs, tile)

    for i in range(1, n):
        to = lax.rem(me + i, n)
        copy = remote(fb.at[to], rows.at[me, c], sx.at[to], rx.at[me], {"sp": to})
        copy.start()
        sent.append(copy)
    copy = remote(fb.at[me], rows.at[me, c], sxc.at[me], rxc.at[me], partner)
    copy.start()
    sent.append(copy)
    rows[me, c] = fb[me]
    for i in range(1, n):
        j = lax.rem(me + n - i, n)
        remote(fb.at[j], rows.at[j, c], sx.at[j], rx.at[j], {"sp": j}).wait_recv()
        copy = remote(rows.at[j, c], rows.at[j, c], sxc.at[j], rxc.at[j], partner)
        copy.start()
        sent.append(copy)
    for i in range(n):
        j = lax.rem(me + n - i, n)
        remote(rows.at[j, 1 - c], rows.at[j, 1 - c], sxc.at[j], rxc.at[j], partner).wait_recv()

    for load in loads[1:]:
        load.wait()
    step = max(1, min(n, 256 // (2 * hs)))

    @pl.loop(0, n // step)
    def _(g):
        here = pl.ds(g * step, step)
        taken = rows[here].reshape(step * 2 * hs, width)
        gated = mm(taken, wg[...], 1, 0)
        lifted = mm(taken, wu[...], 1, 0)
        hidden = (gated * jax.nn.sigmoid(gated) * lifted).astype(BF16)

        @pl.loop(0, width // 512)
        def _(i):
            at = pl.ds(pl.multiple_of(i * 512, 512), 512)
            piece = mm(hidden, wd[:, at], 1, 0).astype(BF16)
            pb[here, :, :, at] = piece.reshape(step, 2, hs, 512)

    for i in range(1, n + 1):
        j = lax.rem(me + i, n)
        copy = remote(pb.at[j, 1 - c], r4.at[j], s4.at[j], q4.at[j], partner)
        copy.start()
        sent.append(copy)
    for i in range(1, n + 1):
        j = lax.rem(me + i, n)
        remote(pb.at[j, c], r4.at[j], s4.at[j], q4.at[j], partner).wait_recv()
        both = (pb[j, c].astype(F32) + r4[j].astype(F32)).astype(BF16)
        if i == n:
            r5[me] = both
        else:
            hb[j] = both
            copy = remote(hb.at[j], r5.at[me], s5.at[j], q5.at[me], {"sp": j})
            copy.start()
            sent.append(copy)
    for i in range(1, n):
        j = lax.rem(me + n - i, n)
        remote(hb.at[j], r5.at[j], s5.at[j], q5.at[j], {"sp": j}).wait_recv()

    @pl.loop(0, width // tile)
    def _(i):
        at = pl.ds(pl.multiple_of(i * tile, tile), tile)
        piece = mm(wcomb[...], r5[:, :, at].reshape(n * hs, tile), 1, 0).astype(BF16)
        part[:, :, :, at] = piece.reshape(ny, 2, rows_here, tile)

    routed = scatter_sum(part, t1, th, t2, st1, rt1, st2, rt2, y, c, ny, sent)
    out[...] = (mid[...] + routed).astype(BF16)
    for copy in sent:
        copy.wait_send()


def solution(mesh):
    n, nt = mesh.shape["sp"], mesh.shape["tp"]
    ny = nt // 2

    def body(
        stream_in, queries, key_rows, values, decay_low, decay_matrix, decay_bias, decay_shift,
        head_gain, output_matrix, feed_gain, routes, route_weights, expert_gate, specialist_widen,
        expert_down,
    ):
        length, keys = queries.shape
        vals = values.shape[1]
        rows_here, width = stream_in.shape
        hidden = expert_gate.shape[2]
        capacity = nt * max(1, TOP * length // (n * nt))
        hs = capacity // 2
        blocks = length // BLK
        vm = pltpu.VMEM
        dma = pltpu.SemaphoreType.DMA
        scratch = [
            vm((length, keys), F32), vm((max(1, blocks - 1), HV, keys), BF16),
            vm((n, HV // n, keys), BF16), vm((n, HV // n, keys), BF16),
            vm((n, HV // n, keys), BF16), vm((n, HV // n, keys), BF16),
            vm((1, keys), F32), vm((n, 1, keys), F32),
            vm((length, vals), F32), vm((length, keys), BF16),
            vm(output_matrix.shape, BF16), vm((width, hidden), BF16), vm((width, hidden), BF16),
            vm((hidden, width), BF16), vm((length, vals), BF16),
            vm((ny, 2, rows_here, width), BF16), vm((ny, rows_here, width), BF16),
            vm((ny, rows_here, width), BF16), vm((ny, rows_here, width), BF16),
            vm((rows_here, width), F32), vm((ny, 2, rows_here, width), BF16),
            vm((length, n * hs), BF16), vm((length, n * hs), BF16),
            vm((n, hs, width), BF16), vm((n, 2, hs, width), BF16), vm((n, 2, hs, width), BF16),
            vm((n, hs, width), BF16), vm((n, hs, width), BF16), vm((n, hs, width), BF16),
            vm((ny, 2, rows_here, width), BF16), vm((ny, rows_here, width), BF16),
            vm((ny, rows_here, width), BF16), vm((ny, rows_here, width), BF16),
            dma((4,)),
            dma((n,)), dma((n,)), dma((n,)), dma((n,)), dma((n,)), dma((n,)),
            dma((ny,)), dma((ny,)), dma((ny,)), dma((ny,)),
            dma((ny,)), dma((ny,)), dma((ny,)), dma((ny,)),
            dma((n,)), dma((n,)), dma((n,)), dma((n,)),
            dma((n,)), dma((n,)), dma((n,)), dma((n,)),
            dma((ny,)), dma((ny,)), dma((ny,)), dma((ny,)),
        ]
        near = pl.BlockSpec(memory_space=pltpu.VMEM)
        far = pl.BlockSpec(memory_space=pl.ANY)
        return pl.pallas_call(
            functools.partial(layer_kernel, n, nt, hs),
            out_shape=jax.ShapeDtypeStruct((rows_here, width), BF16),
            in_specs=[near] * 9 + [far] + [near] * 3 + [far] * 3,
            out_specs=near,
            scratch_shapes=scratch,
            compiler_params=pltpu.CompilerParams(
                collective_id=0, has_side_effects=True, vmem_limit_bytes=64_000_000
            ),
            name="layer",
        )(
            stream_in, queries, key_rows, values, decay_low, decay_matrix, decay_bias.reshape(1, -1),
            decay_shift, head_gain.reshape(1, -1), output_matrix, feed_gain.reshape(1, -1), routes,
            route_weights, expert_gate, specialist_widen, expert_down,
        )

    return jax.shard_map(
        body,
        mesh=mesh,
        in_specs=(
            P(("sp", "tp"), None), P("sp", "tp"), P("sp", "tp"), P("sp", "tp"), P("sp", None),
            P(None, "tp"), P("tp"), P("sp", "tp"), P(), P("tp", None), P(), P("sp", None),
            P("sp", None), P("sp", None, "tp"), P("sp", None, "tp"), P("sp", "tp", None),
        ),
        out_specs=P(("sp", "tp"), None),
        check_vma=False,
    )
```

```python
import functools

import jax
import jax.numpy as jnp
from jax import lax
from jax.experimental import pallas as pl
from jax.experimental.pallas import tpu as pltpu
from jax.sharding import PartitionSpec as P

HK = 256
HV = 512
TOP = 2
BLK = 128
TEMPER = 16.0
EPSILON = 1e-06
HIGHEST = lax.Precision.HIGHEST
MESH = pl.DeviceIdType.MESH
F32 = jnp.float32
BF16 = jnp.bfloat16


def mm(a, b, ca, cb, precision=None):
    return lax.dot_general(
        a, b, (((ca,), (cb,)), ((), ())), preferred_element_type=F32, precision=precision
    )


def remote(src, dst, send, recv, target):
    return pltpu.make_async_remote_copy(
        src_ref=src, dst_ref=dst, send_sem=send, recv_sem=recv, device_id=target, device_id_type=MESH
    )


def scatter_sum(src, r1, half, r2, s1, q1, s2, q2, y, c, ny, sent):
    partner = {"tp": 2 * y + 1 - c}
    for i in range(1, ny + 1):
        to = lax.rem(y + i, ny)
        copy = remote(src.at[to, 1 - c], r1.at[to], s1.at[to], q1.at[to], partner)
        copy.start()
        sent.append(copy)
    for i in range(1, ny):
        to = lax.rem(y + i, ny)
        remote(src.at[to, c], r1.at[to], s1.at[to], q1.at[to], partner).wait_recv()
        half[to] = (src[to, c].astype(F32) + r1[to].astype(F32)).astype(BF16)
        copy = remote(half.at[to], r2.at[y], s2.at[to], q2.at[y], {"tp": 2 * to + c})
        copy.start()
        sent.append(copy)
    remote(src.at[y, c], r1.at[y], s1.at[y], q1.at[y], partner).wait_recv()
    total = src[y, c].astype(F32) + r1[y].astype(F32)
    for i in range(1, ny):
        to = lax.rem(y + i, ny)
        remote(half.at[to], r2.at[to], s2.at[to], q2.at[to], {"tp": 2 * to + c}).wait_recv()
        total = total + r2[to].astype(F32)
    return total


def layer_kernel(
    n, nt, hs, size, yl,
    stream, q, k, v, low, mat, bias, shift, gain, wout, fgain, routes, rweights, wgate, wup, wdown,
    out,
    ins, prior, sbuf, rbuf, cbuf, carry, tsend, trecv, dec, decall, acc, qs,
    wo, wg, wu, wd, mixed,
    prod, p1, ph, p2, mid, group, selt, wcomb, fb, rows, pb, r4, hy, r6, hb, r5, part, t1, th, t2,
    wsem, sa, ra, sd, rd, sb, rb, stt, rtt, sp1, rp1, sp2, rp2, sg, rg, sgc, rgc, sx, rx, sy, ry, sxc, rxc,
    s4, q4, s6, q6, s5, q5, st1, rt1, st2, rt2,
):
    me = lax.axis_index("sp")
    t = lax.axis_index("tp")
    y = t // 2
    c = lax.rem(t, 2)
    ny = nt // 2
    mine, team, teams = lax.rem(me, size), me // size, n // size
    first_one = team * size
    yo = y if yl > 1 else 0
    part_of = 2 * yo + c
    partner = {"tp": 2 * y + 1 - c}
    length = q.shape[0]
    heads = q.shape[1] // HK
    blocks = length // BLK
    width = stream.shape[1]
    rows_here = stream.shape[0]
    sent = []

    barrier = pltpu.get_barrier_semaphore()
    for i in range(1, n):
        pl.semaphore_signal(barrier, inc=1, device_id={"sp": lax.rem(me + i, n)}, device_id_type=MESH)
    for i in range(1, ny):
        pl.semaphore_signal(
            barrier, inc=1, device_id={"tp": 2 * lax.rem(y + i, ny) + c}, device_id_type=MESH
        )
    pl.semaphore_signal(barrier, inc=1, device_id=partner, device_id_type=MESH)

    loads = [
        pltpu.make_async_copy(wout, wo, wsem.at[0]),
        pltpu.make_async_copy(wgate.at[0], wg, wsem.at[1]),
        pltpu.make_async_copy(wup.at[0], wu, wsem.at[2]),
        pltpu.make_async_copy(wdown.at[0], wd, wsem.at[3]),
    ]
    for load in loads:
        load.start()

    row_id = lax.broadcasted_iota(jnp.int32, (BLK, BLK), 0)
    col_id = lax.broadcasted_iota(jnp.int32, (BLK, BLK), 1)
    causal = row_id >= col_id
    tril = causal.astype(F32)

    shifts = shift[...].T

    for h in range(heads):
        ks = slice(h * HK, (h + 1) * HK)
        pre = mm(low[...], mat[:, ks], 0, 0) + bias[:, ks]
        logged = (jnp.minimum(pre, 0.0) - jnp.log1p(jnp.exp(-jnp.abs(pre)))) / TEMPER + shifts[:, h : h + 1]
        whole = None
        for b in range(blocks):
            at = slice(b * BLK, (b + 1) * BLK)
            inside = mm(tril, logged[at], 1, 0, HIGHEST)
            ins[at, ks] = inside
            last = inside[BLK - 1 : BLK, :]
            whole = last if whole is None else whole + last
        dec[:, ks] = jnp.exp(whole)
    decall[mine] = dec[...]

    for h in range(heads):
        ks, vs = slice(h * HK, (h + 1) * HK), slice(h * HV, (h + 1) * HV)
        state = None
        for b in range(blocks):
            at = slice(b * BLK, (b + 1) * BLK)
            inside = ins[at, ks]
            last = inside[BLK - 1 : BLK, :]
            end = (k[at, ks].astype(F32) * jnp.exp(last - inside)).astype(BF16)
            added = mm(v[at, vs], end, 0, 0)
            state = added if state is None else state * jnp.exp(last) + added
            if b < blocks - 1:
                prior[b, :, ks] = state.astype(BF16)
        sbuf[h] = state.astype(BF16).reshape(size, HV // size, HK)
        if h == 0:
            pl.semaphore_wait(barrier, n - 1 + ny - 1 + 1)
            for i in range(1, size):
                to = lax.rem(mine + i, size)
                copy = remote(dec, decall.at[mine], sd.at[to], rd.at[mine], {"sp": first_one + to})
                copy.start()
                sent.append(copy)
        for i in range(1, size):
            to = lax.rem(mine + i, size)
            copy = remote(
                sbuf.at[h, to], rbuf.at[h, mine], sa.at[h, to], ra.at[h, mine], {"sp": first_one + to}
            )
            copy.start()
            sent.append(copy)
        rbuf[h, mine] = sbuf[h, mine]

    for i in range(1, size):
        j = lax.rem(mine + i, size)
        remote(dec, decall.at[j], sd.at[j], rd.at[j], {"sp": first_one + j}).wait_recv()
    onward = {"sp": lax.rem(me + size, n)}
    for h in range(heads):
        ks, vs = slice(h * HK, (h + 1) * HK), slice(h * HV, (h + 1) * HV)
        for i in range(1, size):
            j = lax.rem(mine + i, size)
            remote(sbuf.at[h, j], rbuf.at[h, j], sa.at[h, j], ra.at[h, j], {"sp": first_one + j}).wait_recv()
        link = remote(tsend.at[h], trecv.at[h], stt.at[h], rtt.at[h], onward)

        @pl.when(team > 0)
        def _():
            link.wait_recv()

        @pl.when(team == 0)
        def _():
            trecv[h] = jnp.zeros_like(trecv[h])

        total = trecv[h].astype(F32)
        for j in range(size):
            cbuf[h, j] = total.astype(BF16)
            total = total * decall[j][:, ks] + rbuf[h, j].astype(F32)

        @pl.when(team < teams - 1)
        def _():
            tsend[h] = total.astype(BF16)
            link.start()

        for i in range(1, size):
            j = lax.rem(mine + i, size)
            remote(
                cbuf.at[h, j], carry.at[h, mine], sb.at[h, j], rb.at[h, mine], {"sp": first_one + j}
            ).start()
        carry[h, mine] = cbuf[h, mine]

        passed = None
        for b in range(blocks):
            at = slice(b * BLK, (b + 1) * BLK)
            inside = ins[at, ks]
            last = inside[BLK - 1 : BLK, :]
            centre = last * 0.5
            qf = q[at, ks].astype(F32) * HK ** (-0.5)
            sq = (qf * jnp.exp(inside - centre)).astype(BF16)
            sk = (k[at, ks].astype(F32) * jnp.exp(centre - inside)).astype(BF16)
            scores = jnp.where(causal, mm(sq, sk, 1, 1), 0.0).astype(BF16)
            local = mm(scores, v[at, vs], 1, 0)
            full = inside if passed is None else inside + passed
            qs[at, ks] = (qf * jnp.exp(full)).astype(BF16)
            if b > 0:
                local = local + mm((qf * jnp.exp(inside)).astype(BF16), prior[b - 1, :, ks], 1, 1)
            passed = last if passed is None else passed + last
            acc[at, vs] = local

    lane = lax.broadcasted_iota(jnp.int32, (length, n), 1).astype(F32)
    named = routes[...].astype(F32).T
    shares = rweights[...].T
    first = (named[:, 0:1] == lane).astype(F32)
    second = (named[:, 1:2] == lane).astype(F32)
    earlier = (
        lax.broadcasted_iota(jnp.int32, (length, length), 0)
        > lax.broadcasted_iota(jnp.int32, (length, length), 1)
    ).astype(BF16)
    counts = mm(earlier, (first + second).astype(BF16), 1, 0)
    slot_lane = lax.broadcasted_iota(jnp.int32, (length, n * hs), 1).astype(F32)
    base = (part_of * hs).astype(F32)
    chosen = jnp.zeros((length, n * hs), F32)
    weighted = jnp.zeros((length, n * hs), F32)
    for j, mask in enumerate((first, second)):
        rank = jnp.sum(counts * mask, axis=1, keepdims=True) - base
        place = jnp.where(
            (rank >= 0) & (rank < hs), named[:, j : j + 1] * hs + rank, -1.0
        )
        hit = place == slot_lane
        chosen = chosen + jnp.where(hit, 1.0, 0.0)
        weighted = weighted + jnp.where(hit, shares[:, j : j + 1], 0.0)
    selt[...] = chosen.astype(BF16)
    wcomb[...] = weighted.astype(BF16)

    for h in range(heads):
        ks, vs = slice(h * HK, (h + 1) * HK), slice(h * HV, (h + 1) * HV)
        for i in range(1, size):
            j = lax.rem(mine + i, size)
            remote(cbuf.at[h, j], carry.at[h, j], sb.at[h, j], rb.at[h, j], {"sp": first_one + j}).wait()
        x = acc[:, vs] + mm(qs[:, ks], carry[h].reshape(HV, HK), 1, 1)
        scale = lax.rsqrt(jnp.mean(x * x, axis=-1, keepdims=True) + EPSILON)
        mixed[:, vs] = (x * scale * gain[...]).astype(BF16)

    loads[0].wait()
    tile = 256

    @pl.loop(0, width // tile)
    def _(i):
        at = pl.ds(pl.multiple_of(i * tile, tile), tile)
        piece = mm(mixed[...], wo[:, at], 1, 0).astype(BF16)
        prod[:, :, :, at] = piece.reshape(ny, 2, rows_here, tile)

    attended = scatter_sum(prod, p1, ph, p2, sp1, rp1, sp2, rp2, y, c, ny, sent)
    midstream = stream[...].astype(F32) + attended
    mid[...] = midstream
    scale = lax.rsqrt(jnp.mean(midstream * midstream, axis=-1, keepdims=True) + EPSILON)
    group[y, c] = (midstream * scale * fgain[...]).astype(BF16)

    for i in range(1, ny):
        to = lax.rem(y + i, ny)
        copy = remote(group.at[y, c], group.at[y, c], sg.at[to], rg.at[y], {"tp": 2 * to + c})
        copy.start()
        sent.append(copy)
    copy = remote(group.at[y, c], group.at[y, c], sgc.at[y], rgc.at[y], partner)
    copy.start()
    sent.append(copy)
    for i in range(1, ny):
        to = lax.rem(y + i, ny)
        remote(group.at[to, c], group.at[to, c], sg.at[to], rg.at[to], {"tp": 2 * to + c}).wait_recv()
        copy = remote(group.at[to, c], group.at[to, c], sgc.at[to], rgc.at[to], partner)
        copy.start()
        sent.append(copy)
    for i in range(ny):
        to = lax.rem(y + i, ny)
        remote(group.at[to, 1 - c], group.at[to, 1 - c], sgc.at[to], rgc.at[to], partner).wait_recv()

    @pl.loop(0, width // tile)
    def _(i):
        at = pl.ds(pl.multiple_of(i * tile, tile), tile)
        picked = mm(selt[...], group[:, :, :, at].reshape(length, tile), 0, 0)
        fb[:, :, at] = picked.astype(BF16).reshape(n, hs, tile)

    def pass_on(i):
        if i > 0:
            remote(fb.at[me], rows.at[i, part_of], sx.at[i], rx.at[i], {"sp": me_at(i)}).wait_recv()
        block = fb.at[me] if i == 0 else rows.at[i, part_of]
        for d in range(1, yl):
            copy = remote(
                block, rows.at[i, part_of], sy.at[i, d], ry.at[i, d], {"tp": 2 * lax.rem(y + d, ny) + c}
            )
            copy.start()
            sent.append(copy)
        copy = remote(block, rows.at[i, part_of], sxc.at[i, yo], rxc.at[i, yo], partner)
        copy.start()
        sent.append(copy)

    def pass_over(i):
        for d in range(1, yl):
            other = lax.rem(y + ny - d, ny)
            block = rows.at[i, 2 * other + c]
            remote(block, block, sy.at[i, d], ry.at[i, d], {"tp": 2 * other + c}).wait_recv()
            copy = remote(block, block, sxc.at[i, other], rxc.at[i, other], partner)
            copy.start()
            sent.append(copy)

    def me_at(i):
        return lax.rem(me + i, n)

    for i in range(1, n):
        to = lax.rem(me + i, n)
        copy = remote(fb.at[to], rows.at[i, part_of], sx.at[i], rx.at[i], {"sp": to})
        copy.start()
        sent.append(copy)
    pass_on(0)
    rows[0, part_of] = fb[me]
    for i in range(1, n):
        pass_on(i)
        pass_over(i - 1)
    pass_over(n - 1)
    for i in range(n):
        for d in range(yl):
            block = rows.at[i, 2 * d + 1 - c]
            remote(block, block, sxc.at[i, d], rxc.at[i, d], partner).wait_recv()

    for load in loads[1:]:
        load.wait()
    parts = 2 * yl
    step = max(1, min(n, 256 // (parts * hs)))
    for g in range(n // step):
        taken = rows[g * step : (g + 1) * step].reshape(step * parts * hs, width)
        gated = mm(taken, wg[...], 1, 1)
        lifted = mm(taken, wu[...], 1, 1)
        hidden = (gated * jax.nn.sigmoid(gated) * lifted).astype(BF16)

        @pl.loop(0, width // 512)
        def _(i):
            at = pl.ds(pl.multiple_of(i * 512, 512), 512)
            piece = mm(hidden, wd[:, at], 1, 0).astype(BF16)
            pb[g * step : (g + 1) * step, :, :, :, at] = piece.reshape(step, yl, 2, hs, 512)

        for i in range(g * step, (g + 1) * step):
            for d in range(yl):
                copy = remote(pb.at[i, d, 1 - c], r4.at[i, d], s4.at[i, d], q4.at[i, d], partner)
                copy.start()
                sent.append(copy)

    def over_core(i):
        for d in range(yl):
            remote(pb.at[i, d, c], r4.at[i, d], s4.at[i, d], q4.at[i, d], partner).wait_recv()
        for d in range(1, yl):
            other = lax.rem(y + d, ny)
            hy[i, other] = (pb[i, other, c].astype(F32) + r4[i, other].astype(F32)).astype(BF16)
            copy = remote(hy.at[i, other], r6.at[i, d], s6.at[i, d], q6.at[i, d], {"tp": 2 * other + c})
            copy.start()
            sent.append(copy)

    def over_y(i):
        both = pb[i, yo, c].astype(F32) + r4[i, yo].astype(F32)
        for d in range(1, yl):
            other = lax.rem(y + ny - d, ny)
            remote(hy.at[i, 0], r6.at[i, d], s6.at[i, d], q6.at[i, d], {"tp": 2 * other + c}).wait_recv()
            both = both + r6[i, d].astype(F32)
        if i == 0:
            r5[me] = both.astype(BF16)
        else:
            j = lax.rem(me + n - i, n)
            hb[i] = both.astype(BF16)
            copy = remote(hb.at[i], r5.at[me], s5.at[j], q5.at[me], {"sp": j})
            copy.start()
            sent.append(copy)

    lag = 2
    order = list(range(1, n)) + [0]
    for at_step in range(n + lag):
        if at_step < n:
            over_core(order[at_step])
        if at_step >= lag:
            over_y(order[at_step - lag])
    for i in range(1, n):
        j = lax.rem(me + n - i, n)
        remote(hb.at[i], r5.at[j], s5.at[j], q5.at[j], {"sp": j}).wait_recv()

    @pl.loop(0, width // tile)
    def _(i):
        at = pl.ds(pl.multiple_of(i * tile, tile), tile)
        piece = mm(wcomb[...], r5[:, :, at].reshape(n * hs, tile), 1, 0).astype(BF16)
        part[:, :, :, at] = piece.reshape(ny, 2, rows_here, tile)

    routed = scatter_sum(part, t1, th, t2, st1, rt1, st2, rt2, y, c, ny, sent)
    out[...] = (mid[...] + routed).astype(BF16)
    for copy in sent:
        copy.wait_send()

    @pl.when(team < teams - 1)
    def _():
        for h in range(heads):
            remote(tsend.at[h], trecv.at[h], stt.at[h], rtt.at[h], onward).wait_send()


def solution(mesh):
    n, nt = mesh.shape["sp"], mesh.shape["tp"]
    ny = nt // 2

    def body(
        stream_in, queries, key_rows, values, decay_low, decay_matrix, decay_bias, decay_shift,
        head_gain, output_matrix, feed_gain, routes, route_weights, expert_gate, specialist_widen,
        expert_down,
    ):
        length, keys = queries.shape
        vals = values.shape[1]
        rows_here, width = stream_in.shape
        hidden = expert_gate.shape[2]
        capacity = nt * max(1, TOP * length // (n * nt))
        yl = ny if capacity // nt >= 8 else 1
        hs = capacity // (2 * yl)
        size = next(x for x in (4, 2, 1) if n % x == 0)
        heads = keys // HK
        blocks = length // BLK
        vm = pltpu.VMEM
        dma = pltpu.SemaphoreType.DMA
        scratch = [
            vm((length, keys), F32), vm((max(1, blocks - 1), HV, keys), BF16),
            *[vm((heads, size, HV // size, HK), BF16)] * 4,
            *[vm((heads, HV // size, HK), BF16)] * 2,
            vm((1, keys), F32), vm((size, 1, keys), F32),
            vm((length, vals), F32), vm((length, keys), BF16),
            vm(output_matrix.shape, BF16), vm((hidden, width), BF16), vm((hidden, width), BF16),
            vm((hidden, width), BF16), vm((length, vals), BF16),
            vm((ny, 2, rows_here, width), BF16), vm((ny, rows_here, width), BF16),
            vm((ny, rows_here, width), BF16), vm((ny, rows_here, width), BF16),
            vm((rows_here, width), F32), vm((ny, 2, rows_here, width), BF16),
            vm((length, n * hs), BF16), vm((length, n * hs), BF16),
            vm((n, hs, width), BF16), vm((n, 2 * yl, hs, width), BF16),
            vm((n, yl, 2, hs, width), BF16), vm((n, yl, hs, width), BF16),
            vm((n, yl, hs, width), BF16), vm((n, yl, hs, width), BF16),
            vm((n, hs, width), BF16), vm((n, hs, width), BF16),
            vm((ny, 2, rows_here, width), BF16), vm((ny, rows_here, width), BF16),
            vm((ny, rows_here, width), BF16), vm((ny, rows_here, width), BF16),
            dma((4,)),
            dma((heads, size)), dma((heads, size)), dma((size,)), dma((size,)),
            dma((heads, size)), dma((heads, size)), dma((heads,)), dma((heads,)),
            dma((ny,)), dma((ny,)), dma((ny,)), dma((ny,)),
            dma((ny,)), dma((ny,)), dma((ny,)), dma((ny,)),
            dma((n,)), dma((n,)), *[dma((n, yl))] * 4,
            *[dma((n, yl))] * 4, dma((n,)), dma((n,)),
            dma((ny,)), dma((ny,)), dma((ny,)), dma((ny,)),
        ]
        near = pl.BlockSpec(memory_space=pltpu.VMEM)
        far = pl.BlockSpec(memory_space=pl.ANY)
        return pl.pallas_call(
            functools.partial(layer_kernel, n, nt, hs, size, yl),
            out_shape=jax.ShapeDtypeStruct((rows_here, width), BF16),
            in_specs=[near] * 9 + [far] + [near] * 3 + [far] * 3,
            out_specs=near,
            scratch_shapes=scratch,
            compiler_params=pltpu.CompilerParams(
                collective_id=0, has_side_effects=True, vmem_limit_bytes=64_000_000
            ),
            name="layer",
        )(
            stream_in, queries, key_rows, values, decay_low.T, decay_matrix, decay_bias.reshape(1, -1),
            decay_shift.T, head_gain.reshape(1, -1), output_matrix, feed_gain.reshape(1, -1), routes.T,
            route_weights.T, expert_gate.swapaxes(1, 2), specialist_widen.swapaxes(1, 2), expert_down,
        )

    return jax.shard_map(
        body,
        mesh=mesh,
        in_specs=(
            P(("sp", "tp"), None), P("sp", "tp"), P("sp", "tp"), P("sp", "tp"), P("sp", None),
            P(None, "tp"), P("tp"), P("sp", "tp"), P(), P("tp", None), P(), P("sp", None),
            P("sp", None), P("sp", None, "tp"), P("sp", None, "tp"), P("sp", "tp", None),
        ),
        out_specs=P(("sp", "tp"), None),
        check_vma=False,
    )
```

```python
import functools

import jax
import jax.numpy as jnp
from jax import lax
from jax.experimental import pallas as pl
from jax.experimental.pallas import tpu as pltpu
from jax.sharding import PartitionSpec as P

HK = 256
HV = 512
TOP = 2
BLK = 128
TEMPER = 16.0
EPSILON = 1e-06
HIGHEST = lax.Precision.HIGHEST
MESH = pl.DeviceIdType.MESH
F32 = jnp.float32
BF16 = jnp.bfloat16


def mm(a, b, ca, cb, precision=None):
    return lax.dot_general(
        a, b, (((ca,), (cb,)), ((), ())), preferred_element_type=F32, precision=precision
    )


def remote(src, dst, send, recv, target):
    return pltpu.make_async_remote_copy(
        src_ref=src, dst_ref=dst, send_sem=send, recv_sem=recv, device_id=target, device_id_type=MESH
    )


def scatter_sum(fill, store, src, r1, half, r2, s1, q1, s2, q2, y, c, ny, sent):
    partner = {"tp": 2 * y + 1 - c}
    width = src.shape[-1]
    sides = [(f, slice(f * width // 2, (f + 1) * width // 2)) for f in range(2)]

    def first(to, f, at):
        return remote(src.at[to, 1 - c, :, at], r1.at[to, :, at], s1.at[f, to], q1.at[f, to], partner)

    def second(to, slot, f, at):
        return remote(
            half.at[to, :, at], r2.at[slot, :, at], s2.at[f, to], q2.at[f, slot], {"tp": 2 * to + c}
        )

    for f, at in sides:
        fill(f)
        for i in range(1, ny + 1):
            copy = first(lax.rem(y + i, ny), f, at)
            copy.start()
            sent.append(copy)
    for f, at in sides:
        for i in range(1, ny):
            to = lax.rem(y + i, ny)
            first(to, f, at).wait_recv()
            half[to, :, at] = (src[to, c, :, at].astype(F32) + r1[to, :, at].astype(F32)).astype(BF16)
            copy = second(to, y, f, at)
            copy.start()
            sent.append(copy)
    for f, at in sides:
        first(y, f, at).wait_recv()
        total = src[y, c, :, at].astype(F32) + r1[y, :, at].astype(F32)
        for i in range(1, ny):
            to = lax.rem(y + i, ny)
            second(to, to, f, at).wait_recv()
            total = total + r2[to, :, at].astype(F32)
        store(at, total)


def layer_kernel(
    n, nt, hs, size, yl,
    stream, q, k, v, low, mat, bias, shift, gain, wout, fgain, routes, rweights, wgate, wup, wdown,
    out,
    ins, prior, sbuf, rbuf, cbuf, carry, tsend, trecv, dec, decall, acc, qs,
    wo, wg, wu, wd, mixed,
    prod, p1, ph, p2, mid, group, selt, wcomb, fb, rows, pb, r4, hy, r6, hb, r5, part, t1, th, t2,
    wsem, sa, ra, sd, rd, sb, rb, stt, rtt, sp1, rp1, sp2, rp2, sg, rg, sgc, rgc, sx, rx, sy, ry, sxc, rxc,
    s4, q4, s6, q6, s5, q5, st1, rt1, st2, rt2,
):
    me = lax.axis_index("sp")
    t = lax.axis_index("tp")
    y = t // 2
    c = lax.rem(t, 2)
    ny = nt // 2
    mine, team, teams = lax.rem(me, size), me // size, n // size
    first_one = team * size
    yo = y if yl > 1 else 0
    part_of = 2 * yo + c
    partner = {"tp": 2 * y + 1 - c}
    length = q.shape[0]
    heads = q.shape[1] // HK
    blocks = length // BLK
    width = stream.shape[1]
    rows_here = stream.shape[0]
    sent = []

    barrier = pltpu.get_barrier_semaphore()
    for i in range(1, n):
        pl.semaphore_signal(barrier, inc=1, device_id={"sp": lax.rem(me + i, n)}, device_id_type=MESH)
    for i in range(1, ny):
        pl.semaphore_signal(
            barrier, inc=1, device_id={"tp": 2 * lax.rem(y + i, ny) + c}, device_id_type=MESH
        )
    pl.semaphore_signal(barrier, inc=1, device_id=partner, device_id_type=MESH)

    loads = [
        pltpu.make_async_copy(wout, wo, wsem.at[0]),
        pltpu.make_async_copy(wgate.at[0], wg, wsem.at[1]),
        pltpu.make_async_copy(wup.at[0], wu, wsem.at[2]),
        pltpu.make_async_copy(wdown.at[0], wd, wsem.at[3]),
    ]
    for load in loads:
        load.start()

    row_id = lax.broadcasted_iota(jnp.int32, (BLK, BLK), 0)
    col_id = lax.broadcasted_iota(jnp.int32, (BLK, BLK), 1)
    causal = row_id >= col_id
    tril = causal.astype(F32)

    shifts = shift[...].T

    for h in range(heads):
        ks = slice(h * HK, (h + 1) * HK)
        pre = mm(low[...], mat[:, ks], 0, 0) + bias[:, ks]
        logged = (jnp.minimum(pre, 0.0) - jnp.log1p(jnp.exp(-jnp.abs(pre)))) / TEMPER + shifts[:, h : h + 1]
        whole = None
        for b in range(blocks):
            at = slice(b * BLK, (b + 1) * BLK)
            inside = mm(tril, logged[at], 1, 0, HIGHEST)
            ins[at, ks] = inside
            last = inside[BLK - 1 : BLK, :]
            whole = last if whole is None else whole + last
        dec[:, ks] = jnp.exp(whole)
    decall[mine] = dec[...]

    for h in range(heads):
        ks, vs = slice(h * HK, (h + 1) * HK), slice(h * HV, (h + 1) * HV)
        state = None
        for b in range(blocks):
            at = slice(b * BLK, (b + 1) * BLK)
            inside = ins[at, ks]
            last = inside[BLK - 1 : BLK, :]
            end = (k[at, ks].astype(F32) * jnp.exp(last - inside)).astype(BF16)
            added = mm(v[at, vs], end, 0, 0)
            state = added if state is None else state * jnp.exp(last) + added
            if b < blocks - 1:
                prior[b, :, ks] = state.astype(BF16)
        sbuf[h] = state.astype(BF16).reshape(size, HV // size, HK)
        if h == 0:
            pl.semaphore_wait(barrier, n - 1 + ny - 1 + 1)
            for i in range(1, size):
                to = lax.rem(mine + i, size)
                copy = remote(dec, decall.at[mine], sd.at[to], rd.at[mine], {"sp": first_one + to})
                copy.start()
                sent.append(copy)
        for i in range(1, size):
            to = lax.rem(mine + i, size)
            copy = remote(
                sbuf.at[h, to], rbuf.at[h, mine], sa.at[h, to], ra.at[h, mine], {"sp": first_one + to}
            )
            copy.start()
            sent.append(copy)
        rbuf[h, mine] = sbuf[h, mine]

    for i in range(1, size):
        j = lax.rem(mine + i, size)
        remote(dec, decall.at[j], sd.at[j], rd.at[j], {"sp": first_one + j}).wait_recv()
    onward = {"sp": lax.rem(me + size, n)}
    for h in range(heads):
        ks, vs = slice(h * HK, (h + 1) * HK), slice(h * HV, (h + 1) * HV)
        for i in range(1, size):
            j = lax.rem(mine + i, size)
            remote(sbuf.at[h, j], rbuf.at[h, j], sa.at[h, j], ra.at[h, j], {"sp": first_one + j}).wait_recv()
        link = remote(tsend.at[h], trecv.at[h], stt.at[h], rtt.at[h], onward)

        @pl.when(team > 0)
        def _():
            link.wait_recv()

        @pl.when(team == 0)
        def _():
            trecv[h] = jnp.zeros_like(trecv[h])

        total = trecv[h].astype(F32)
        for j in range(size):
            cbuf[h, j] = total.astype(BF16)
            total = total * decall[j][:, ks] + rbuf[h, j].astype(F32)

        @pl.when(team < teams - 1)
        def _():
            tsend[h] = total.astype(BF16)
            link.start()

        for i in range(1, size):
            j = lax.rem(mine + i, size)
            remote(
                cbuf.at[h, j], carry.at[h, mine], sb.at[h, j], rb.at[h, mine], {"sp": first_one + j}
            ).start()
        carry[h, mine] = cbuf[h, mine]

        passed = None
        for b in range(blocks):
            at = slice(b * BLK, (b + 1) * BLK)
            inside = ins[at, ks]
            last = inside[BLK - 1 : BLK, :]
            centre = last * 0.5
            qf = q[at, ks].astype(F32) * HK ** (-0.5)
            sq = (qf * jnp.exp(inside - centre)).astype(BF16)
            sk = (k[at, ks].astype(F32) * jnp.exp(centre - inside)).astype(BF16)
            scores = jnp.where(causal, mm(sq, sk, 1, 1), 0.0).astype(BF16)
            local = mm(scores, v[at, vs], 1, 0)
            full = inside if passed is None else inside + passed
            qs[at, ks] = (qf * jnp.exp(full)).astype(BF16)
            if b > 0:
                local = local + mm((qf * jnp.exp(inside)).astype(BF16), prior[b - 1, :, ks], 1, 1)
            passed = last if passed is None else passed + last
            acc[at, vs] = local

    lane = lax.broadcasted_iota(jnp.int32, (length, n), 1).astype(F32)
    named = routes[...].astype(F32).T
    shares = rweights[...].T
    first = (named[:, 0:1] == lane).astype(F32)
    second = (named[:, 1:2] == lane).astype(F32)
    earlier = (
        lax.broadcasted_iota(jnp.int32, (length, length), 0)
        > lax.broadcasted_iota(jnp.int32, (length, length), 1)
    ).astype(BF16)
    counts = mm(earlier, (first + second).astype(BF16), 1, 0)
    slot_lane = lax.broadcasted_iota(jnp.int32, (length, n * hs), 1).astype(F32)
    base = (part_of * hs).astype(F32)
    chosen = jnp.zeros((length, n * hs), F32)
    weighted = jnp.zeros((length, n * hs), F32)
    for j, mask in enumerate((first, second)):
        rank = jnp.sum(counts * mask, axis=1, keepdims=True) - base
        place = jnp.where(
            (rank >= 0) & (rank < hs), named[:, j : j + 1] * hs + rank, -1.0
        )
        hit = place == slot_lane
        chosen = chosen + jnp.where(hit, 1.0, 0.0)
        weighted = weighted + jnp.where(hit, shares[:, j : j + 1], 0.0)
    selt[...] = chosen.astype(BF16)
    wcomb[...] = weighted.astype(BF16)

    for h in range(heads):
        ks, vs = slice(h * HK, (h + 1) * HK), slice(h * HV, (h + 1) * HV)
        for i in range(1, size):
            j = lax.rem(mine + i, size)
            remote(cbuf.at[h, j], carry.at[h, j], sb.at[h, j], rb.at[h, j], {"sp": first_one + j}).wait()
        x = acc[:, vs] + mm(qs[:, ks], carry[h].reshape(HV, HK), 1, 1)
        scale = lax.rsqrt(jnp.mean(x * x, axis=-1, keepdims=True) + EPSILON)
        mixed[:, vs] = (x * scale * gain[...]).astype(BF16)

    loads[0].wait()
    tile = 256

    def project(f):
        @pl.loop(f * (width // tile // 2), (f + 1) * (width // tile // 2))
        def _(i):
            at = pl.ds(pl.multiple_of(i * tile, tile), tile)
            piece = mm(mixed[...], wo[:, at], 1, 0).astype(BF16)
            prod[:, :, :, at] = piece.reshape(ny, 2, rows_here, tile)

    def add_stream(at, total):
        mid[:, at] = stream[:, at].astype(F32) + total

    scatter_sum(project, add_stream, prod, p1, ph, p2, sp1, rp1, sp2, rp2, y, c, ny, sent)
    midstream = mid[...]
    scale = lax.rsqrt(jnp.mean(midstream * midstream, axis=-1, keepdims=True) + EPSILON)
    group[y, c] = (midstream * scale * fgain[...]).astype(BF16)

    for i in range(1, ny):
        to = lax.rem(y + i, ny)
        copy = remote(group.at[y, c], group.at[y, c], sg.at[to], rg.at[y], {"tp": 2 * to + c})
        copy.start()
        sent.append(copy)
    copy = remote(group.at[y, c], group.at[y, c], sgc.at[y], rgc.at[y], partner)
    copy.start()
    sent.append(copy)
    for i in range(1, ny):
        to = lax.rem(y + i, ny)
        remote(group.at[to, c], group.at[to, c], sg.at[to], rg.at[to], {"tp": 2 * to + c}).wait_recv()
        copy = remote(group.at[to, c], group.at[to, c], sgc.at[to], rgc.at[to], partner)
        copy.start()
        sent.append(copy)
    for i in range(ny):
        to = lax.rem(y + i, ny)
        remote(group.at[to, 1 - c], group.at[to, 1 - c], sgc.at[to], rgc.at[to], partner).wait_recv()

    @pl.loop(0, width // tile)
    def _(i):
        at = pl.ds(pl.multiple_of(i * tile, tile), tile)
        picked = mm(selt[...], group[:, :, :, at].reshape(length, tile), 0, 0)
        fb[:, :, at] = picked.astype(BF16).reshape(n, hs, tile)

    def pass_on(i):
        if i > 0:
            remote(fb.at[me], rows.at[i, part_of], sx.at[i], rx.at[i], {"sp": me_at(i)}).wait_recv()
        block = fb.at[me] if i == 0 else rows.at[i, part_of]
        for d in range(1, yl):
            copy = remote(
                block, rows.at[i, part_of], sy.at[i, d], ry.at[i, d], {"tp": 2 * lax.rem(y + d, ny) + c}
            )
            copy.start()
            sent.append(copy)
        copy = remote(block, rows.at[i, part_of], sxc.at[i, yo], rxc.at[i, yo], partner)
        copy.start()
        sent.append(copy)

    def pass_over(i):
        for d in range(1, yl):
            other = lax.rem(y + ny - d, ny)
            block = rows.at[i, 2 * other + c]
            remote(block, block, sy.at[i, d], ry.at[i, d], {"tp": 2 * other + c}).wait_recv()
            copy = remote(block, block, sxc.at[i, other], rxc.at[i, other], partner)
            copy.start()
            sent.append(copy)

    def me_at(i):
        return lax.rem(me + i, n)

    for i in range(1, n):
        to = lax.rem(me + i, n)
        copy = remote(fb.at[to], rows.at[i, part_of], sx.at[i], rx.at[i], {"sp": to})
        copy.start()
        sent.append(copy)
    parts = 2 * yl
    step = max(1, min(n, 256 // (parts * hs)))

    def experts(g):
        for i in range(g * step, (g + 1) * step):
            for d in range(yl):
                block = rows.at[i, 2 * d + 1 - c]
                remote(block, block, sxc.at[i, d], rxc.at[i, d], partner).wait_recv()
        taken = rows[g * step : (g + 1) * step].reshape(step * parts * hs, width)
        gated = mm(taken, wg[...], 1, 1)
        lifted = mm(taken, wu[...], 1, 1)
        hidden = (gated * jax.nn.sigmoid(gated) * lifted).astype(BF16)

        @pl.loop(0, width // 512)
        def _(i):
            at = pl.ds(pl.multiple_of(i * 512, 512), 512)
            piece = mm(hidden, wd[:, at], 1, 0).astype(BF16)
            pb[g * step : (g + 1) * step, :, :, :, at] = piece.reshape(step, yl, 2, hs, 512)

        for i in range(g * step, (g + 1) * step):
            for d in range(yl):
                copy = remote(pb.at[i, d, 1 - c], r4.at[i, d], s4.at[i, d], q4.at[i, d], partner)
                copy.start()
                sent.append(copy)

    pass_on(0)
    rows[0, part_of] = fb[me]
    early = min(step + 1, n - 1)
    for load in loads[1:]:
        load.wait()
    for i in range(1, n):
        pass_on(i)
        pass_over(i - 1)
        if i == early and step < n:
            experts(0)
    pass_over(n - 1)
    for g in range(1 if step < n else 0, n // step):
        experts(g)

    def over_core(i):
        for d in range(yl):
            remote(pb.at[i, d, c], r4.at[i, d], s4.at[i, d], q4.at[i, d], partner).wait_recv()
        for d in range(1, yl):
            other = lax.rem(y + d, ny)
            hy[i, other] = (pb[i, other, c].astype(F32) + r4[i, other].astype(F32)).astype(BF16)
            copy = remote(hy.at[i, other], r6.at[i, d], s6.at[i, d], q6.at[i, d], {"tp": 2 * other + c})
            copy.start()
            sent.append(copy)

    def over_y(i):
        both = pb[i, yo, c].astype(F32) + r4[i, yo].astype(F32)
        for d in range(1, yl):
            other = lax.rem(y + ny - d, ny)
            remote(hy.at[i, 0], r6.at[i, d], s6.at[i, d], q6.at[i, d], {"tp": 2 * other + c}).wait_recv()
            both = both + r6[i, d].astype(F32)
        if i == 0:
            r5[me] = both.astype(BF16)
        else:
            j = lax.rem(me + n - i, n)
            hb[i] = both.astype(BF16)
            copy = remote(hb.at[i], r5.at[me], s5.at[j], q5.at[me], {"sp": j})
            copy.start()
            sent.append(copy)

    lag = 2
    order = list(range(1, n)) + [0]
    for at_step in range(n + lag):
        if at_step < n:
            over_core(order[at_step])
        if at_step >= lag:
            over_y(order[at_step - lag])
    for i in range(1, n):
        j = lax.rem(me + n - i, n)
        remote(hb.at[i], r5.at[j], s5.at[j], q5.at[j], {"sp": j}).wait_recv()

    def combine(f):
        @pl.loop(f * (width // tile // 2), (f + 1) * (width // tile // 2))
        def _(i):
            at = pl.ds(pl.multiple_of(i * tile, tile), tile)
            piece = mm(wcomb[...], r5[:, :, at].reshape(n * hs, tile), 1, 0).astype(BF16)
            part[:, :, :, at] = piece.reshape(ny, 2, rows_here, tile)

    def add_routed(at, total):
        out[:, at] = (mid[:, at] + total).astype(BF16)

    scatter_sum(combine, add_routed, part, t1, th, t2, st1, rt1, st2, rt2, y, c, ny, sent)
    for copy in sent:
        copy.wait_send()

    @pl.when(team < teams - 1)
    def _():
        for h in range(heads):
            remote(tsend.at[h], trecv.at[h], stt.at[h], rtt.at[h], onward).wait_send()


def solution(mesh):
    n, nt = mesh.shape["sp"], mesh.shape["tp"]
    ny = nt // 2

    def body(
        stream_in, queries, key_rows, values, decay_low, decay_matrix, decay_bias, decay_shift,
        head_gain, output_matrix, feed_gain, routes, route_weights, expert_gate, specialist_widen,
        expert_down,
    ):
        length, keys = queries.shape
        vals = values.shape[1]
        rows_here, width = stream_in.shape
        hidden = expert_gate.shape[2]
        capacity = nt * max(1, TOP * length // (n * nt))
        yl = ny if capacity // nt >= 8 else 1
        hs = capacity // (2 * yl)
        size = next(x for x in (4, 2, 1) if n % x == 0)
        heads = keys // HK
        blocks = length // BLK
        vm = pltpu.VMEM
        dma = pltpu.SemaphoreType.DMA
        scratch = [
            vm((length, keys), F32), vm((max(1, blocks - 1), HV, keys), BF16),
            *[vm((heads, size, HV // size, HK), BF16)] * 4,
            *[vm((heads, HV // size, HK), BF16)] * 2,
            vm((1, keys), F32), vm((size, 1, keys), F32),
            vm((length, vals), F32), vm((length, keys), BF16),
            vm(output_matrix.shape, BF16), vm((hidden, width), BF16), vm((hidden, width), BF16),
            vm((hidden, width), BF16), vm((length, vals), BF16),
            vm((ny, 2, rows_here, width), BF16), vm((ny, rows_here, width), BF16),
            vm((ny, rows_here, width), BF16), vm((ny, rows_here, width), BF16),
            vm((rows_here, width), F32), vm((ny, 2, rows_here, width), BF16),
            vm((length, n * hs), BF16), vm((length, n * hs), BF16),
            vm((n, hs, width), BF16), vm((n, 2 * yl, hs, width), BF16),
            vm((n, yl, 2, hs, width), BF16), vm((n, yl, hs, width), BF16),
            vm((n, yl, hs, width), BF16), vm((n, yl, hs, width), BF16),
            vm((n, hs, width), BF16), vm((n, hs, width), BF16),
            vm((ny, 2, rows_here, width), BF16), vm((ny, rows_here, width), BF16),
            vm((ny, rows_here, width), BF16), vm((ny, rows_here, width), BF16),
            dma((4,)),
            dma((heads, size)), dma((heads, size)), dma((size,)), dma((size,)),
            dma((heads, size)), dma((heads, size)), dma((heads,)), dma((heads,)),
            *[dma((2, ny))] * 4, *[dma((ny,))] * 4,
            dma((n,)), dma((n,)), *[dma((n, yl))] * 4,
            *[dma((n, yl))] * 4, dma((n,)), dma((n,)),
            *[dma((2, ny))] * 4,
        ]
        near = pl.BlockSpec(memory_space=pltpu.VMEM)
        far = pl.BlockSpec(memory_space=pl.ANY)
        return pl.pallas_call(
            functools.partial(layer_kernel, n, nt, hs, size, yl),
            out_shape=jax.ShapeDtypeStruct((rows_here, width), BF16),
            in_specs=[near] * 9 + [far] + [near] * 3 + [far] * 3,
            out_specs=near,
            scratch_shapes=scratch,
            compiler_params=pltpu.CompilerParams(
                collective_id=0, has_side_effects=True, vmem_limit_bytes=64_000_000
            ),
            name="layer",
        )(
            stream_in, queries, key_rows, values, decay_low.T, decay_matrix, decay_bias.reshape(1, -1),
            decay_shift.T, head_gain.reshape(1, -1), output_matrix, feed_gain.reshape(1, -1), routes.T,
            route_weights.T, expert_gate.swapaxes(1, 2), specialist_widen.swapaxes(1, 2), expert_down,
        )

    return jax.shard_map(
        body,
        mesh=mesh,
        in_specs=(
            P(("sp", "tp"), None), P("sp", "tp"), P("sp", "tp"), P("sp", "tp"), P("sp", None),
            P(None, "tp"), P("tp"), P("sp", "tp"), P(), P("tp", None), P(), P("sp", None),
            P("sp", None), P("sp", None, "tp"), P("sp", None, "tp"), P("sp", "tp", None),
        ),
        out_specs=P(("sp", "tp"), None),
        check_vma=False,
    )
```
